32 devices in a mesh: rep: 2 (over x), fs: 8 (over z, y), tp: 2 (over core).
Axes of the slice: x: 2, y: 2, z: 4, core: 2. Of those that a mesh axis runs over, the one named last changes fastest.
Arguments:
- tokens: bfloat16 [4096, 1024], P(('rep', 'fs', 'tp')), may hold values from -4 to 4
- mixer_out: bfloat16 [4096, 1024], P(('rep', 'fs')), may hold values from -4 to 4
- gain_first: float32 [1024], replicated, may hold values from 0.1 to 1.9
- gate_first: bfloat16 [1024, 2816], P('fs', 'tp'), may hold values from -0.1875 to 0.1875
- up_first: bfloat16 [1024, 2816], P('fs', 'tp'), may hold values from -0.1875 to 0.1875
- down_first: bfloat16 [2816, 1024], P('tp', 'fs'), may hold values from -0.109375 to 0.109375
- gain_second: float32 [1024], replicated, may hold values from 0.1 to 1.9
- gate_second: bfloat16 [1024, 2816], P('fs', 'tp'), may hold values from -0.1875 to 0.1875
- up_second: bfloat16 [1024, 2816], P('fs', 'tp'), may hold values from -0.1875 to 0.1875
- down_second: bfloat16 [2816, 1024], P('tp', 'fs'), may hold values from -0.109375 to 0.109375
- gain_last: float32 [1024], P('tp'), may hold values from 0.1 to 1.9
Outputs:
- result: bfloat16 [4096, 1024], P(('rep', 'fs'), 'tp')
The draws below stay inside these ranges and needn't reach their ends.
All inputs are finite; a program needn't handle non-finite values.
Results may differ from the reference program's by a relative error of at most 0.02.
Values may be sent and summed in bfloat16 or wider, within the bound.
A program may use at most 64 MiB of HBM per device.

```python
import jax
import jax.numpy as jnp
from jax import lax

D = 1024
FF = 2816
TOKENS = 4096
N_TP = 2


def level_of(stream_key, shape, cuts, smallest, largest):
    def one(axis_at, parts):
        steps = jax.random.uniform(jax.random.fold_in(jax.random.fold_in(stream_key, 6), axis_at), (parts,), jnp.float32, smallest / len(cuts), largest / len(cuts))
        return jnp.repeat(jnp.exp(steps), shape[axis_at] // parts).reshape((-1,) + (1,) * (len(shape) - axis_at - 1))

    level = one(*cuts[0])
    for cut in cuts[1:]:
        level = level * one(*cut)
    return level


def gaussian(stream_key, extent, width, bound, pieces=(), held_as=jnp.bfloat16):
    array = jax.random.normal(stream_key, extent, jnp.float32) * width
    if len(pieces) > 0:
        array = level_of(stream_key, extent, pieces, -0.22, 0.18) * array
    return jnp.clip(array, min=-bound, max=bound).astype(held_as)


def setup_inputs(seed: int = 0) -> dict:
    seeds = jax.random.split(jax.random.key(seed), 12)
    return {
        "tokens": gaussian(seeds[0], (TOKENS, D), 0.3, 4.0, ((0, 32),)),
        "mixer_out": gaussian(seeds[1], (TOKENS, D), 0.3, 4.0, ((0, 16),)),
        "gain_first": jnp.clip(1.0 + 0.18 * jax.random.normal(seeds[2], (D,), jnp.float32), 0.1, 1.9),
        "gate_first": gaussian(seeds[3], (D, FF), D ** -0.5, 0.1875, ((0, 8), (1, 2))),
        "up_first": gaussian(seeds[4], (D, FF), D ** -0.5, 0.1875, ((0, 8), (1, 2))),
        "down_first": gaussian(seeds[5], (FF, D), FF ** -0.5, 0.109375, ((0, 2), (1, 8))),
        "gain_second": jnp.clip(1.0 + 0.18 * jax.random.normal(seeds[6], (D,), jnp.float32), 0.1, 1.9),
        "gate_second": gaussian(seeds[7], (D, FF), D ** -0.5, 0.1875, ((0, 8), (1, 2))),
        "up_second": gaussian(seeds[8], (D, FF), D ** -0.5, 0.1875, ((0, 8), (1, 2))),
        "down_second": gaussian(seeds[9], (FF, D), FF ** -0.5, 0.109375, ((0, 2), (1, 8))),
        "gain_last": jnp.clip(1.0 + 0.18 * jax.random.normal(seeds[10], (D,), jnp.float32), 0.1, 1.9),
    }


EPS = 1e-06

def normalize(floats_in, gain_vec):
    floats = floats_in.astype(jnp.float32)
    factor = lax.rsqrt(lax.optimization_barrier(jnp.mean(floats * floats, axis=-1, keepdims=True)) + EPS)
    return (floats * factor * gain_vec.astype(jnp.float32)).astype(jnp.bfloat16)

def half_mlp(normed, w_gate, w_up, w_down):
    gate_acc = jnp.dot(normed, w_gate, preferred_element_type=jnp.float32)
    up_acc = jnp.dot(normed, w_up, preferred_element_type=jnp.float32)
    hidden = (jax.nn.silu(gate_acc) * up_acc).astype(jnp.bfloat16)
    block_size = FF // N_TP
    summed = jnp.zeros((normed.shape[0], w_down.shape[1]), jnp.float32)
    for block_idx in range(N_TP):
        lower = block_idx * block_size
        partial_sum = jnp.dot(hidden[:, lower:lower + block_size], w_down[lower:lower + block_size], preferred_element_type=jnp.float32).astype(jnp.bfloat16)
        partial_sum = lax.optimization_barrier(partial_sum)
        summed = summed + partial_sum.astype(jnp.float32)
    return summed

def reference(tokens, mixer_out, gain_first, gate_first, up_first, down_first, gain_second, gate_second, up_second, down_second, gain_last):
    ffn_one = half_mlp(normalize(tokens, gain_first), gate_first, up_first, down_first)
    after_one = (tokens.astype(jnp.float32) + 0.5 * ffn_one).astype(jnp.bfloat16)
    mixed_in = (after_one.astype(jnp.float32) + mixer_out.astype(jnp.float32)).astype(jnp.bfloat16)
    ffn_two = half_mlp(normalize(mixed_in, gain_second), gate_second, up_second, down_second)
    after_two = (mixed_in.astype(jnp.float32) + 0.5 * ffn_two).astype(jnp.bfloat16)
    return normalize(after_two, gain_last)
```

```python
import functools

import jax
import jax.numpy as jnp
from jax import lax
from jax.experimental import pallas as pl
from jax.experimental.pallas import tpu as pltpu
from jax.sharding import PartitionSpec as P

EPS = 1e-06


def over_all(slab, axis, dim):

    def gathered(part):
        return lax.all_gather(part, axis, axis=dim, tiled=True)

    return jax.tree.map(gathered, slab)


def normalize(floats_in, gain_vec):
    floats = floats_in.astype(jnp.float32)
    factor = lax.rsqrt(jnp.mean(floats * floats, axis=-1, keepdims=True) + EPS)
    return (floats * factor * gain_vec.astype(jnp.float32)).astype(jnp.bfloat16)


def gather_group(row_block):
    return lax.all_gather(row_block, "tp", axis=0, tiled=True)


def inner_hidden(normed, w_gate, w_up):

    def add_both(totals, pieces):
        columns = lax.slice_in_dim(normed, 0, pieces[0].shape[0], axis=1)
        return (
            totals[0] + jnp.dot(columns, pieces[0], preferred_element_type=jnp.float32),
            totals[1] + jnp.dot(columns, pieces[1], preferred_element_type=jnp.float32),
        )

    empty = jnp.zeros((normed.shape[0], w_gate.shape[1]), jnp.float32)
    gate_acc, up_acc = add_both((empty, empty), over_all((w_gate, w_up), "fs", 0))
    return (jax.nn.silu(gate_acc) * up_acc).astype(jnp.bfloat16)


def outer_weight(w_down):
    return lax.all_gather(w_down, "fs", axis=1, tiled=True)


def local(
    tokens,
    mixer_out,
    gain_first,
    gate_first,
    up_first,
    down_first,
    gain_second,
    gate_second,
    up_second,
    down_second,
    gain_last,
):
    rows_dev = tokens.shape[0]
    tp_count = lax.axis_size("tp")
    tp_index = lax.axis_index("tp")
    normed_own = normalize(tokens, gain_first)
    normed_one = gather_group(normed_own)
    hidden_one = inner_hidden(normed_one, gate_first, up_first)
    down_full = outer_weight(down_first)

    def row_terms():
        picked = lax.slice_in_dim(hidden_one, 0, rows_dev * lax.axis_size("tp"), axis=0)
        return jnp.dot(picked, down_full, preferred_element_type=jnp.float32)

    ffn_one = lax.psum_scatter(
        row_terms().astype(jnp.bfloat16), "tp", scatter_dimension=0, tiled=True
    ).astype(jnp.float32)
    after_one = (tokens.astype(jnp.float32) + 0.5 * ffn_one).astype(jnp.bfloat16)
    own_mixer = lax.dynamic_slice_in_dim(mixer_out, tp_index * rows_dev, rows_dev, 0)
    mixed_in = (after_one.astype(jnp.float32) + own_mixer.astype(jnp.float32)).astype(jnp.bfloat16)
    gathered = gather_group(mixed_in)
    normed_two = normalize(gathered, gain_second)
    hidden_two = inner_hidden(normed_two, gate_second, up_second)
    down_two_full = outer_weight(down_second)
    terms_two = jnp.dot(hidden_two, down_two_full, preferred_element_type=jnp.float32)
    ffn_two = lax.psum_scatter(
        terms_two.astype(jnp.bfloat16), "tp", scatter_dimension=1, tiled=True
    ).astype(jnp.float32)
    col_width = ffn_two.shape[1]
    my_cols = lax.dynamic_slice_in_dim(gathered, tp_index * col_width, col_width, 1)
    after_two = (my_cols.astype(jnp.float32) + 0.5 * ffn_two).astype(jnp.bfloat16)
    floats = after_two.astype(jnp.float32)
    sum_sq = lax.psum(jnp.sum(floats * floats, axis=1), "tp")
    factor = lax.rsqrt(sum_sq / (col_width * tp_count) + EPS)
    return (floats * factor[:, None] * gain_last.astype(jnp.float32)[None, :]).astype(jnp.bfloat16)


MESH = pl.DeviceIdType.MESH
PLANE = 4
LANES = 128


def fits(mesh):
    return mesh.shape["rep"] == 2 and mesh.shape["tp"] == 2 and mesh.shape["fs"] % 2 == 0 and mesh.shape["fs"] >= 2


def norm_rows(floats, gain_row):
    factor = lax.rsqrt(jnp.mean(floats * floats, axis=-1, keepdims=True) + EPS)
    return (floats * factor * gain_row).astype(jnp.bfloat16)


def kernel(
    depth, width, overlap,
    tok, mix, gain1, gain2, gain3, g1, u1, d1, g2, u2, d2,
    out,
    xs, mixed, normed, hid, gu, dw, outgoing, arrived, own, result, landed,
    local_sem, y_send, up_send, down_send, wide_recv, core_send, core_recv,
    row_send, row_recv, end_sem,
):
    rep, fs, tp = lax.axis_index("rep"), lax.axis_index("fs"), lax.axis_index("tp")
    z, y = fs // 2, fs % 2
    rows, width_all = tok.shape
    block = g1.shape[0]
    weights = (g1, u1, d1, g2, u2, d2)
    partner = (rep, fs, 1 - tp)

    def relative(k):
        return ((rep + k // 2) % 2, 2 * z + (y + k % 2) % 2, tp)

    up, down = (rep, fs + 2, tp), (rep, fs - 2, tp)

    barrier = pltpu.get_barrier_semaphore()

    def greet(device):
        pl.semaphore_signal(barrier, inc=1, device_id=device, device_id_type=MESH)

    for k in range(1, PLANE):
        greet(relative(k))
    greet(partner)

    @pl.when(z > 0)
    def _():
        greet(down)

    @pl.when(z < depth - 1)
    def _():
        greet(up)

    below, above = (z + depth - 1) // depth, (2 * depth - 2 - z) // depth
    pl.semaphore_wait(barrier, PLANE + below + above)

    def quarter(which_y):
        q = 2 * rep + which_y
        return q * width - (q // (PLANE - 1)) * overlap

    def own_part(m, which_y):
        at = pl.ds(pl.multiple_of(quarter(which_y), LANES), width)
        return weights[m].at[at, :] if m % 3 == 2 else weights[m].at[:, at]

    def place(m, blk, half):
        at = pl.ds(pl.multiple_of(blk * block, block), block)
        if m % 3 == 2:
            return dw.at[m // 3, half, :, at]
        return gu.at[m // 3, m % 3, half, at, :]

    def remote(src, dst, send, recv, device):
        return pltpu.make_async_remote_copy(
            src_ref=src, dst_ref=dst, send_sem=send, recv_sem=recv, device_id=device, device_id_type=MESH
        )

    def keep(m):
        return pltpu.make_async_copy(own_part(m, y), place(m, fs, tp), local_sem.at[m])

    def swap(m):
        return remote(own_part(m, 1 - y), place(m, fs, tp), y_send.at[m], wide_recv.at[m, fs], relative(1))

    def send_up(m, blk, src):
        return remote(src, place(m, blk, tp), up_send.at[m, blk], wide_recv.at[m, blk], up)

    def send_down(m, blk, src):
        return remote(src, place(m, blk, tp), down_send.at[m, blk], wide_recv.at[m, blk], down)

    def send_core(m, blk, src):
        return remote(src, place(m, blk, tp), core_send.at[m, blk], core_recv.at[m, blk], partner)

    def came(m, blk):
        remote(place(m, blk, tp), place(m, blk, tp), core_send.at[m, blk], wide_recv.at[m, blk], partner).wait_recv()

    def came_core(m, blk):
        there = place(m, blk, 1 - tp)
        remote(there, there, core_send.at[m, blk], core_recv.at[m, blk], partner).wait_recv()

    def spread(m, blk, src, go_up=True, go_down=True):
        if go_up:

            @pl.when(z < depth - 1)
            def _():
                send_up(m, blk, src).start()

        if go_down:

            @pl.when(z > 0)
            def _():
                send_down(m, blk, src).start()

        send_core(m, blk, src).start()

    def begin(group):
        for m in group:
            keep(m).start()
            spread(m, fs, own_part(m, y))

    def from_side(group):
        other = 2 * z + (1 - y)
        for m in group:
            came(m, other)
            spread(m, other, place(m, other, tp))

    def from_line(group, d):
        for side in (y, 1 - y):
            for m in group:

                @pl.when(z >= d)
                def _():
                    blk = 2 * (z - d) + side
                    came(m, blk)
                    spread(m, blk, place(m, blk, tp), go_down=False)

                @pl.when(z + d < depth)
                def _():
                    blk = 2 * (z + d) + side
                    came(m, blk)
                    spread(m, blk, place(m, blk, tp), go_up=False)

    def ready(group):
        for m in group:
            keep(m).wait()
            for blk in range(2 * depth):
                came_core(m, blk)

    def rows_to(phase, k, src, dst):
        return remote(src, dst, row_send.at[phase, k], row_recv.at[phase, k], relative(k))

    def normalize_all(first, rest, gain):
        gain_row = gain[...]

        def chunk(i, carry):
            normed[pl.ds(i * rows, rows), :] = norm_rows(rest[i].astype(jnp.float32), gain_row)
            return carry

        normed[pl.ds(0, rows), :] = norm_rows(first.astype(jnp.float32), gain_row)
        lax.fori_loop(1, PLANE, chunk, 0)

    def multiply(layer):
        lanes = lax.broadcasted_iota(jnp.int32, (2 * rows, width), 1)
        counted = lanes >= overlap * ((2 * rep + y) // (PLANE - 1))

        def inner(i, carry):
            half, at = i // 2, pl.ds(pl.multiple_of((i % 2) * 2 * rows, 2 * rows), 2 * rows)
            columns = normed[at, :]
            gate = jnp.dot(columns, gu[layer, 0, half], preferred_element_type=jnp.float32)
            value = jnp.dot(columns, gu[layer, 1, half], preferred_element_type=jnp.float32)
            hidden = gate / (1.0 + jnp.exp(-gate)) * value
            hid[half, at, :] = jnp.where(counted, hidden, 0.0).astype(jnp.bfloat16)
            return carry

        lax.fori_loop(0, 4, inner, 0)
        for k in range(PLANE - 1, -1, -1):
            at = pl.ds(k * rows, rows)
            part = jnp.dot(hid[0, at, :], dw[layer, 0], preferred_element_type=jnp.float32)
            part = part + jnp.dot(hid[1, at, :], dw[layer, 1], preferred_element_type=jnp.float32)
            if k:
                outgoing[layer, k] = part.astype(jnp.bfloat16)
                rows_to(1 + 2 * layer, k, outgoing.at[layer, k], arrived.at[layer, k]).start()
            else:
                own[...] = part

    def rows_came(phase, dst):
        for k in range(1, PLANE):
            rows_to(phase, k, dst.at[k], dst.at[k]).wait_recv()

    def total(layer):
        summed = own[...]
        for k in range(1, PLANE):
            summed = summed + arrived[layer, k].astype(jnp.float32)
        return summed

    one, two = (0, 1, 2), (3, 4, 5)
    for m in one:
        swap(m).start()
    begin(one)
    for k in (3, 2, 1):
        rows_to(0, k, tok, xs.at[k]).start()
    for m in two:
        swap(m).start()
    from_side(one)
    for d in range(1, depth):
        from_line(one, d)
    begin(two)
    from_side(two)
    rows_came(0, xs)
    normalize_all(tok[...], xs, gain1)
    ready(one)
    multiply(0)
    if depth > 1:
        from_line(two, 1)
    rows_came(1, arrived.at[0])
    after_one = (tok[...].astype(jnp.float32) + 0.5 * total(0)).astype(jnp.bfloat16)
    own_mix = mix[pl.ds(pl.multiple_of(tp * rows, rows), rows), :]
    mixed[0] = (after_one.astype(jnp.float32) + own_mix.astype(jnp.float32)).astype(jnp.bfloat16)
    for k in (3, 2, 1):
        rows_to(2, k, mixed.at[0], mixed.at[k]).start()
    for d in range(2, depth):
        from_line(two, d)
    rows_came(2, mixed)
    normalize_all(mixed[0], mixed, gain2)
    ready(two)
    multiply(1)
    rows_came(3, arrived.at[1])
    after_two = (mixed[0].astype(jnp.float32) + 0.5 * total(1)).astype(jnp.bfloat16)
    final = norm_rows(after_two.astype(jnp.float32), gain3[...])
    share = width_all // 2
    result[0] = final[:, :share]
    result[1] = final[:, share:]
    over = remote(result.at[1 - tp], landed, end_sem.at[0], end_sem.at[1], partner)
    over.start()
    out[pl.ds(pl.multiple_of(tp * rows, rows), rows), :] = result[tp]

    for m in range(6):
        swap(m).wait_send()
        for blk in range(2 * depth):
            send_core(m, blk, place(m, blk, tp)).wait_send()

            @pl.when((z < depth - 1) & (blk // 2 <= z))
            def _():
                send_up(m, blk, place(m, blk, tp)).wait_send()

            @pl.when((z > 0) & (blk // 2 >= z))
            def _():
                send_down(m, blk, place(m, blk, tp)).wait_send()

    for phase, src in enumerate((xs, outgoing.at[0], mixed, outgoing.at[1])):
        for k in range(1, PLANE):
            rows_to(phase, k, src.at[k], src.at[k]).wait_send()
    over.wait_send()
    over.wait_recv()
    out[pl.ds(pl.multiple_of((1 - tp) * rows, rows), rows), :] = landed[...]


def fused(
    tokens,
    mixer_out,
    gain_first,
    gate_first,
    up_first,
    down_first,
    gain_second,
    gate_second,
    up_second,
    down_second,
    gain_last,
):
    rows, features = tokens.shape
    block, hidden = gate_first.shape
    blocks = lax.axis_size("fs")
    width = -(-hidden // (PLANE * LANES)) * LANES
    last = lax.all_gather(gain_last, "tp", axis=0, tiled=True)
    vmem, anywhere = pl.BlockSpec(memory_space=pltpu.VMEM), pl.BlockSpec(memory_space=pl.ANY)
    half = jnp.bfloat16
    sems = pltpu.SemaphoreType.DMA
    return pl.pallas_call(
        functools.partial(kernel, blocks // 2, width, PLANE * width - hidden),
        out_shape=jax.ShapeDtypeStruct((2 * rows, features // 2), half),
        in_specs=[vmem] * 5 + [anywhere] * 6,
        out_specs=vmem,
        scratch_shapes=[
            pltpu.VMEM((PLANE, rows, features), half),
            pltpu.VMEM((PLANE, rows, features), half),
            pltpu.VMEM((PLANE * rows, features), half),
            pltpu.VMEM((2, PLANE * rows, width), half),
            pltpu.VMEM((2, 2, 2, features, width), half),
            pltpu.VMEM((2, 2, width, features), half),
            pltpu.VMEM((2, PLANE, rows, features), half),
            pltpu.VMEM((2, PLANE, rows, features), half),
            pltpu.VMEM((rows, features), jnp.float32),
            pltpu.VMEM((2, rows, features // 2), half),
            pltpu.VMEM((rows, features // 2), half),
            sems((6,)),
            sems((6,)),
            sems((6, blocks)),
            sems((6, blocks)),
            sems((6, blocks)),
            sems((6, blocks)),
            sems((6, blocks)),
            sems((4, PLANE)),
            sems((4, PLANE)),
            sems((2,)),
        ],
        compiler_params=pltpu.CompilerParams(
            collective_id=0, has_side_effects=True, vmem_limit_bytes=48 * 1024 * 1024
        ),
    )(
        tokens,
        mixer_out,
        gain_first[None, :],
        gain_second[None, :],
        last[None, :],
        gate_first,
        up_first,
        down_first,
        gate_second,
        up_second,
        down_second,
    )


def solution(mesh):
    in_specs = (
        P(("rep", "fs", "tp"), None),
        P(("rep", "fs"), None),
        P(),
        P("fs", "tp"),
        P("fs", "tp"),
        P("tp", "fs"),
        P(),
        P("fs", "tp"),
        P("fs", "tp"),
        P("tp", "fs"),
        P("tp"),
    )
    out_specs = P(("rep", "fs"), "tp")
    body = fused if fits(mesh) else local
    return jax.shard_map(body, mesh=mesh, in_specs=in_specs, out_specs=out_specs, check_vma=False)
```

```python
import functools

import jax
import jax.numpy as jnp
from jax import lax
from jax.experimental import pallas as pl
from jax.experimental.pallas import tpu as pltpu
from jax.sharding import PartitionSpec as P

EPS = 1e-06


def over_all(slab, axis, dim):

    def gathered(part):
        return lax.all_gather(part, axis, axis=dim, tiled=True)

    return jax.tree.map(gathered, slab)


def normalize(floats_in, gain_vec):
    floats = floats_in.astype(jnp.float32)
    factor = lax.rsqrt(jnp.mean(floats * floats, axis=-1, keepdims=True) + EPS)
    return (floats * factor * gain_vec.astype(jnp.float32)).astype(jnp.bfloat16)


def gather_group(row_block):
    return lax.all_gather(row_block, "tp", axis=0, tiled=True)


def inner_hidden(normed, w_gate, w_up):

    def add_both(totals, pieces):
        columns = lax.slice_in_dim(normed, 0, pieces[0].shape[0], axis=1)
        return (
            totals[0] + jnp.dot(columns, pieces[0], preferred_element_type=jnp.float32),
            totals[1] + jnp.dot(columns, pieces[1], preferred_element_type=jnp.float32),
        )

    empty = jnp.zeros((normed.shape[0], w_gate.shape[1]), jnp.float32)
    gate_acc, up_acc = add_both((empty, empty), over_all((w_gate, w_up), "fs", 0))
    return (jax.nn.silu(gate_acc) * up_acc).astype(jnp.bfloat16)


def outer_weight(w_down):
    return lax.all_gather(w_down, "fs", axis=1, tiled=True)


def local(
    tokens,
    mixer_out,
    gain_first,
    gate_first,
    up_first,
    down_first,
    gain_second,
    gate_second,
    up_second,
    down_second,
    gain_last,
):
    rows_dev = tokens.shape[0]
    tp_count = lax.axis_size("tp")
    tp_index = lax.axis_index("tp")
    normed_own = normalize(tokens, gain_first)
    normed_one = gather_group(normed_own)
    hidden_one = inner_hidden(normed_one, gate_first, up_first)
    down_full = outer_weight(down_first)

    def row_terms():
        picked = lax.slice_in_dim(hidden_one, 0, rows_dev * lax.axis_size("tp"), axis=0)
        return jnp.dot(picked, down_full, preferred_element_type=jnp.float32)

    ffn_one = lax.psum_scatter(
        row_terms().astype(jnp.bfloat16), "tp", scatter_dimension=0, tiled=True
    ).astype(jnp.float32)
    after_one = (tokens.astype(jnp.float32) + 0.5 * ffn_one).astype(jnp.bfloat16)
    own_mixer = lax.dynamic_slice_in_dim(mixer_out, tp_index * rows_dev, rows_dev, 0)
    mixed_in = (after_one.astype(jnp.float32) + own_mixer.astype(jnp.float32)).astype(jnp.bfloat16)
    gathered = gather_group(mixed_in)
    normed_two = normalize(gathered, gain_second)
    hidden_two = inner_hidden(normed_two, gate_second, up_second)
    down_two_full = outer_weight(down_second)
    terms_two = jnp.dot(hidden_two, down_two_full, preferred_element_type=jnp.float32)
    ffn_two = lax.psum_scatter(
        terms_two.astype(jnp.bfloat16), "tp", scatter_dimension=1, tiled=True
    ).astype(jnp.float32)
    col_width = ffn_two.shape[1]
    my_cols = lax.dynamic_slice_in_dim(gathered, tp_index * col_width, col_width, 1)
    after_two = (my_cols.astype(jnp.float32) + 0.5 * ffn_two).astype(jnp.bfloat16)
    floats = after_two.astype(jnp.float32)
    sum_sq = lax.psum(jnp.sum(floats * floats, axis=1), "tp")
    factor = lax.rsqrt(sum_sq / (col_width * tp_count) + EPS)
    return (floats * factor[:, None] * gain_last.astype(jnp.float32)[None, :]).astype(jnp.bfloat16)


MESH = pl.DeviceIdType.MESH
PLANE = 4
LANES = 128


def fits(mesh):
    return mesh.shape["rep"] == 2 and mesh.shape["tp"] == 2 and mesh.shape["fs"] % 2 == 0 and mesh.shape["fs"] >= 2


def norm_rows(floats, gain_row):
    factor = lax.rsqrt(jnp.mean(floats * floats, axis=-1, keepdims=True) + EPS)
    return (floats * factor * gain_row).astype(jnp.bfloat16)


def kernel(
    depth, width, overlap,
    tokens, mixer, gains1, gains2, gains3, g1, u1, d1, g2, u2, d2,
    out,
    mix, gain1, gain2, gain3, xs, mixed, normed, hid, gu, dw, outgoing, arrived, own, result, landed,
    local_sem, y_send, up_send, down_send, wide_recv, core_send, core_recv,
    row_send, row_recv, part_send, part_recv, end_sem,
):
    rep, fs, tp = lax.axis_index("rep"), lax.axis_index("fs"), lax.axis_index("tp")
    z, y = fs // 2, fs % 2
    rows, width_all = tokens.shape
    block = g1.shape[0]
    weights = (g1, u1, d1, g2, u2, d2)
    partner = (rep, fs, 1 - tp)

    def relative(k):
        return ((rep + k // 2) % 2, 2 * z + (y + k % 2) % 2, tp)

    up, down = (rep, fs + 2, tp), (rep, fs - 2, tp)

    own_rows = pl.ds(pl.multiple_of(tp * rows, rows), rows)
    loads = [
        pltpu.make_async_copy(src, dst, local_sem.at[6 + i])
        for i, (src, dst) in enumerate(
            (
                (tokens, xs.at[0]),
                (mixer.at[own_rows, :], mix),
                (gains1, gain1),
                (gains2, gain2),
                (gains3, gain3.at[tp]),
            )
        )
    ]
    for load in loads:
        load.start()

    barrier = pltpu.get_barrier_semaphore()

    def greet(device):
        pl.semaphore_signal(barrier, inc=1, device_id=device, device_id_type=MESH)

    for k in range(1, PLANE):
        greet(relative(k))
    greet(partner)

    @pl.when(z > 0)
    def _():
        greet(down)

    @pl.when(z < depth - 1)
    def _():
        greet(up)

    below, above = (z + depth - 1) // depth, (2 * depth - 2 - z) // depth
    pl.semaphore_wait(barrier, PLANE + below + above)

    def quarter(which_y):
        q = 2 * rep + which_y
        return q * width - (q // (PLANE - 1)) * overlap

    def own_part(m, which_y):
        at = pl.ds(pl.multiple_of(quarter(which_y), LANES), width)
        return weights[m].at[at, :] if m % 3 == 2 else weights[m].at[:, at]

    def place(m, blk, half):
        at = pl.ds(pl.multiple_of(blk * block, block), block)
        if m % 3 == 2:
            return dw.at[m // 3, half, :, at]
        return gu.at[m // 3, m % 3, half, at, :]

    def remote(src, dst, send, recv, device):
        return pltpu.make_async_remote_copy(
            src_ref=src, dst_ref=dst, send_sem=send, recv_sem=recv, device_id=device, device_id_type=MESH
        )

    def keep(m):
        return pltpu.make_async_copy(own_part(m, y), place(m, fs, tp), local_sem.at[m])

    def swap(m):
        return remote(own_part(m, 1 - y), place(m, fs, tp), y_send.at[m], wide_recv.at[m, fs], relative(1))

    def send_up(m, blk, src):
        return remote(src, place(m, blk, tp), up_send.at[m, blk], wide_recv.at[m, blk], up)

    def send_down(m, blk, src):
        return remote(src, place(m, blk, tp), down_send.at[m, blk], wide_recv.at[m, blk], down)

    def send_core(m, blk, src):
        return remote(src, place(m, blk, tp), core_send.at[m, blk], core_recv.at[m, blk], partner)

    def came(m, blk):
        remote(place(m, blk, tp), place(m, blk, tp), core_send.at[m, blk], wide_recv.at[m, blk], partner).wait_recv()

    def came_core(m, blk):
        there = place(m, blk, 1 - tp)
        remote(there, there, core_send.at[m, blk], core_recv.at[m, blk], partner).wait_recv()

    def spread(m, blk, src, go_up=True, go_down=True):
        if go_up:

            @pl.when(z < depth - 1)
            def _():
                send_up(m, blk, src).start()

        if go_down:

            @pl.when(z > 0)
            def _():
                send_down(m, blk, src).start()

        send_core(m, blk, src).start()

    def begin(group):
        for m in group:
            keep(m).start()
            spread(m, fs, own_part(m, y))

    def from_side(group):
        other = 2 * z + (1 - y)
        for m in group:
            came(m, other)
            spread(m, other, place(m, other, tp))

    def from_line(group, d):
        for side in (y, 1 - y):
            for m in group:

                @pl.when(z >= d)
                def _():
                    blk = 2 * (z - d) + side
                    came(m, blk)
                    spread(m, blk, place(m, blk, tp), go_down=False)

                @pl.when(z + d < depth)
                def _():
                    blk = 2 * (z + d) + side
                    came(m, blk)
                    spread(m, blk, place(m, blk, tp), go_up=False)

    def ready(group):
        for m in group:
            keep(m).wait()
            for blk in range(2 * depth):
                came_core(m, blk)

    def rows_to(phase, k, src, dst):
        return remote(src, dst, row_send.at[phase, k], row_recv.at[phase, k], relative(k))

    def normalize_all(source, gain):
        gain_row = gain[...]

        def chunk(i, carry):
            normed[pl.ds(pl.multiple_of(i * rows, rows), rows), :] = norm_rows(source[i].astype(jnp.float32), gain_row)
            return carry

        lax.fori_loop(0, PLANE, chunk, 0)

    def inner(layer):
        lanes = lax.broadcasted_iota(jnp.int32, (2 * rows, width), 1)
        counted = lanes >= overlap * ((2 * rep + y) // (PLANE - 1))

        def piece(i, carry):
            half, at = i // 2, pl.ds(pl.multiple_of((i % 2) * 2 * rows, 2 * rows), 2 * rows)
            columns = normed[at, :]
            gate = jnp.dot(columns, gu[layer, 0, half], preferred_element_type=jnp.float32)
            value = jnp.dot(columns, gu[layer, 1, half], preferred_element_type=jnp.float32)
            hidden = gate / (1.0 + jnp.exp(-gate)) * value
            hid[half, at, :] = jnp.where(counted, hidden, 0.0).astype(jnp.bfloat16)
            return carry

        lax.fori_loop(0, 4, piece, 0)

    def share_of(layer, k, zz):
        at = pl.ds(pl.multiple_of(zz * 2 * block, 2 * block), 2 * block)
        return remote(
            outgoing.at[layer, k, :, at],
            arrived.at[layer, k, :, at],
            part_send.at[layer, k, zz],
            part_recv.at[layer, k, zz],
            relative(k),
        )

    def outer(layer, zz):
        for which in range(2):
            came_core(3 * layer + 2, 2 * zz + which)
        at = pl.ds(pl.multiple_of(zz * 2 * block, 2 * block), 2 * block)
        part = jnp.dot(hid[0], dw[layer, 0, :, at], preferred_element_type=jnp.float32)
        part = part + jnp.dot(hid[1], dw[layer, 1, :, at], preferred_element_type=jnp.float32)
        for k in range(PLANE - 1, -1, -1):
            mine = part[k * rows : (k + 1) * rows]
            if k:
                outgoing[layer, k, :, at] = mine.astype(jnp.bfloat16)
                share_of(layer, k, zz).start()
            else:
                own[:, at] = mine

    def outer_at(layer, d):
        if d == 0:
            keep(3 * layer + 2).wait()
            outer(layer, z)
            return

        @pl.when(z >= d)
        def _():
            outer(layer, z - d)

        @pl.when(z + d < depth)
        def _():
            outer(layer, z + d)

    def rows_came(phase, dst):
        for k in range(1, PLANE):
            rows_to(phase, k, dst.at[k], dst.at[k]).wait_recv()

    def total(layer):
        for k in range(1, PLANE):
            for zz in range(depth):
                share_of(layer, k, zz).wait_recv()
        summed = own[...]
        for k in range(1, PLANE):
            summed = summed + arrived[layer, k].astype(jnp.float32)
        return summed

    one, two = (0, 1, 2), (3, 4, 5)
    swap_gain = remote(gains3, gain3.at[tp], end_sem.at[2], end_sem.at[3], partner)
    for m in one:
        swap(m).start()
    begin(one)
    for k in (3, 2, 1):
        rows_to(0, k, tokens, xs.at[k]).start()
    for m in two:
        swap(m).start()
    swap_gain.start()
    from_side(one)
    for d in range(1, depth):
        from_line(one, d)
    begin(two)
    from_side(two)
    for load in loads:
        load.wait()
    rows_came(0, xs)
    normalize_all(xs, gain1)
    ready(one[:2])
    inner(0)
    for d in range(depth):
        outer_at(0, d)
    if depth > 1:
        from_line(two[:2], 1)
    after_one = (xs[0].astype(jnp.float32) + 0.5 * total(0)).astype(jnp.bfloat16)
    mixed[0] = (after_one.astype(jnp.float32) + mix[...].astype(jnp.float32)).astype(jnp.bfloat16)
    for k in (3, 2, 1):
        rows_to(1, k, mixed.at[0], mixed.at[k]).start()
    for d in range(2, depth - 1):
        from_line(two[:2], d)
    if depth > 2:
        from_line(two[2:], 1)
    rows_came(1, mixed)
    normalize_all(mixed, gain2)
    if depth > 2:
        from_line(two[:2], depth - 1)
    elif depth > 1:
        from_line(two[2:], 1)
    ready(two[:2])
    inner(1)
    outer_at(1, 0)
    for d in range(1, depth):
        if d > 1:
            from_line(two[2:], d)
        outer_at(1, d)
    after_two = (mixed[0].astype(jnp.float32) + 0.5 * total(1)).astype(jnp.bfloat16)
    floats = after_two.astype(jnp.float32)
    floats = floats * lax.rsqrt(jnp.mean(floats * floats, axis=-1, keepdims=True) + EPS)
    share = width_all // 2
    swap_gain.wait_send()
    remote(gain3.at[1 - tp], gain3.at[1 - tp], end_sem.at[2], end_sem.at[3], partner).wait_recv()
    result[0] = (floats[:, :share] * gain3[0]).astype(jnp.bfloat16)
    result[1] = (floats[:, share:] * gain3[1]).astype(jnp.bfloat16)
    over = remote(result.at[1 - tp], landed, end_sem.at[0], end_sem.at[1], partner)
    over.start()
    out[own_rows, :] = result[tp]

    for m in range(6):
        swap(m).wait_send()
        for blk in range(2 * depth):
            send_core(m, blk, place(m, blk, tp)).wait_send()

            @pl.when((z < depth - 1) & (blk // 2 <= z))
            def _():
                send_up(m, blk, place(m, blk, tp)).wait_send()

            @pl.when((z > 0) & (blk // 2 >= z))
            def _():
                send_down(m, blk, place(m, blk, tp)).wait_send()

    for phase, src in enumerate((xs, mixed)):
        for k in range(1, PLANE):
            rows_to(phase, k, src.at[k], src.at[k]).wait_send()
            for zz in range(depth):
                share_of(phase, k, zz).wait_send()
    over.wait_send()
    over.wait_recv()
    out[pl.ds(pl.multiple_of((1 - tp) * rows, rows), rows), :] = landed[...]


def fused(
    tokens,
    mixer_out,
    gain_first,
    gate_first,
    up_first,
    down_first,
    gain_second,
    gate_second,
    up_second,
    down_second,
    gain_last,
):
    rows, features = tokens.shape
    block, hidden = gate_first.shape
    blocks = lax.axis_size("fs")
    width = -(-hidden // (PLANE * LANES)) * LANES
    vmem, anywhere = pl.BlockSpec(memory_space=pltpu.VMEM), pl.BlockSpec(memory_space=pltpu.HBM)
    half = jnp.bfloat16
    sems = pltpu.SemaphoreType.DMA
    return pl.pallas_call(
        functools.partial(kernel, blocks // 2, width, PLANE * width - hidden),
        out_shape=jax.ShapeDtypeStruct((2 * rows, features // 2), half),
        in_specs=[anywhere] * 11,
        out_specs=vmem,
        scratch_shapes=[
            pltpu.VMEM((rows, features), half),
            pltpu.VMEM((1, features), jnp.float32),
            pltpu.VMEM((1, features), jnp.float32),
            pltpu.VMEM((2, 1, features // 2), jnp.float32),
            pltpu.VMEM((PLANE, rows, features), half),
            pltpu.VMEM((PLANE, rows, features), half),
            pltpu.VMEM((PLANE * rows, features), half),
            pltpu.VMEM((2, PLANE * rows, width), half),
            pltpu.VMEM((2, 2, 2, features, width), half),
            pltpu.VMEM((2, 2, width, features), half),
            pltpu.VMEM((2, PLANE, rows, features), half),
            pltpu.VMEM((2, PLANE, rows, features), half),
            pltpu.VMEM((rows, features), jnp.float32),
            pltpu.VMEM((2, rows, features // 2), half),
            pltpu.VMEM((rows, features // 2), half),
            sems((11,)),
            sems((6,)),
            sems((6, blocks)),
            sems((6, blocks)),
            sems((6, blocks)),
            sems((6, blocks)),
            sems((6, blocks)),
            sems((2, PLANE)),
            sems((2, PLANE)),
            sems((2, PLANE, blocks // 2)),
            sems((2, PLANE, blocks // 2)),
            sems((4,)),
        ],
        compiler_params=pltpu.CompilerParams(
            collective_id=0, has_side_effects=True, vmem_limit_bytes=67_043_328
        ),
    )(
        tokens,
        mixer_out,
        gain_first[None, :],
        gain_second[None, :],
        gain_last[None, :],
        gate_first,
        up_first,
        down_first,
        gate_second,
        up_second,
        down_second,
    )


def solution(mesh):
    in_specs = (
        P(("rep", "fs", "tp"), None),
        P(("rep", "fs"), None),
        P(),
        P("fs", "tp"),
        P("fs", "tp"),
        P("tp", "fs"),
        P(),
        P("fs", "tp"),
        P("fs", "tp"),
        P("tp", "fs"),
        P("tp"),
    )
    out_specs = P(("rep", "fs"), "tp")
    body = fused if fits(mesh) else local
    return jax.shard_map(body, mesh=mesh, in_specs=in_specs, out_specs=out_specs, check_vma=False)
```

```python
import functools

import jax
import jax.numpy as jnp
from jax import lax
from jax.experimental import pallas as pl
from jax.experimental.pallas import tpu as pltpu
from jax.sharding import PartitionSpec as P

EPS = 1e-06


def over_all(slab, axis, dim):

    def gathered(part):
        return lax.all_gather(part, axis, axis=dim, tiled=True)

    return jax.tree.map(gathered, slab)


def normalize(floats_in, gain_vec):
    floats = floats_in.astype(jnp.float32)
    factor = lax.rsqrt(jnp.mean(floats * floats, axis=-1, keepdims=True) + EPS)
    return (floats * factor * gain_vec.astype(jnp.float32)).astype(jnp.bfloat16)


def gather_group(row_block):
    return lax.all_gather(row_block, "tp", axis=0, tiled=True)


def inner_hidden(normed, w_gate, w_up):

    def add_both(totals, pieces):
        columns = lax.slice_in_dim(normed, 0, pieces[0].shape[0], axis=1)
        return (
            totals[0] + jnp.dot(columns, pieces[0], preferred_element_type=jnp.float32),
            totals[1] + jnp.dot(columns, pieces[1], preferred_element_type=jnp.float32),
        )

    empty = jnp.zeros((normed.shape[0], w_gate.shape[1]), jnp.float32)
    gate_acc, up_acc = add_both((empty, empty), over_all((w_gate, w_up), "fs", 0))
    return (jax.nn.silu(gate_acc) * up_acc).astype(jnp.bfloat16)


def outer_weight(w_down):
    return lax.all_gather(w_down, "fs", axis=1, tiled=True)


def local(
    tokens,
    mixer_out,
    gain_first,
    gate_first,
    up_first,
    down_first,
    gain_second,
    gate_second,
    up_second,
    down_second,
    gain_last,
):
    rows_dev = tokens.shape[0]
    tp_count = lax.axis_size("tp")
    tp_index = lax.axis_index("tp")
    normed_own = normalize(tokens, gain_first)
    normed_one = gather_group(normed_own)
    hidden_one = inner_hidden(normed_one, gate_first, up_first)
    down_full = outer_weight(down_first)

    def row_terms():
        picked = lax.slice_in_dim(hidden_one, 0, rows_dev * lax.axis_size("tp"), axis=0)
        return jnp.dot(picked, down_full, preferred_element_type=jnp.float32)

    ffn_one = lax.psum_scatter(
        row_terms().astype(jnp.bfloat16), "tp", scatter_dimension=0, tiled=True
    ).astype(jnp.float32)
    after_one = (tokens.astype(jnp.float32) + 0.5 * ffn_one).astype(jnp.bfloat16)
    own_mixer = lax.dynamic_slice_in_dim(mixer_out, tp_index * rows_dev, rows_dev, 0)
    mixed_in = (after_one.astype(jnp.float32) + own_mixer.astype(jnp.float32)).astype(jnp.bfloat16)
    gathered = gather_group(mixed_in)
    normed_two = normalize(gathered, gain_second)
    hidden_two = inner_hidden(normed_two, gate_second, up_second)
    down_two_full = outer_weight(down_second)
    terms_two = jnp.dot(hidden_two, down_two_full, preferred_element_type=jnp.float32)
    ffn_two = lax.psum_scatter(
        terms_two.astype(jnp.bfloat16), "tp", scatter_dimension=1, tiled=True
    ).astype(jnp.float32)
    col_width = ffn_two.shape[1]
    my_cols = lax.dynamic_slice_in_dim(gathered, tp_index * col_width, col_width, 1)
    after_two = (my_cols.astype(jnp.float32) + 0.5 * ffn_two).astype(jnp.bfloat16)
    floats = after_two.astype(jnp.float32)
    sum_sq = lax.psum(jnp.sum(floats * floats, axis=1), "tp")
    factor = lax.rsqrt(sum_sq / (col_width * tp_count) + EPS)
    return (floats * factor[:, None] * gain_last.astype(jnp.float32)[None, :]).astype(jnp.bfloat16)


MESH = pl.DeviceIdType.MESH
PLANE = 4
SUBLANES = 16
LANES = 128
CROSS = (((1,), (1,)), ((), ()))


def fits(mesh):
    return mesh.shape["rep"] == 2 and mesh.shape["tp"] == 2 and mesh.shape["fs"] % 2 == 0


def norm_rows(floats, gain_row):
    factor = lax.rsqrt(jnp.mean(floats * floats, axis=-1, keepdims=True) + EPS)
    return (floats * factor * gain_row).astype(jnp.bfloat16)


def kernel(
    depth, width,
    tokens, mixer, gains1, gains2, gains3, g1, u1, d1, g2, u2, d2,
    out,
    raw, turned, mix, gain1, gain2, gain3, xs, mixed, normed, hid, gu, dw, outgoing, arrived, own, result, landed,
    local_sem, y_send, up_send, down_send, wide_recv, core_send, core_recv,
    row_send, row_recv, part_send, part_recv, end_sem,
):
    rep, fs, tp = lax.axis_index("rep"), lax.axis_index("fs"), lax.axis_index("tp")
    z, y = fs // 2, fs % 2
    rows, width_all = tokens.shape
    block = g1.shape[0]
    weights = (g1, u1, d1, g2, u2, d2)
    partner = (rep, fs, 1 - tp)

    def relative(k):
        return ((rep + k // 2) % 2, 2 * z + (y + k % 2) % 2, tp)

    up, down = (rep, fs + 2, tp), (rep, fs - 2, tp)

    own_rows = pl.ds(pl.multiple_of(tp * rows, rows), rows)
    loads = [
        pltpu.make_async_copy(src, dst, local_sem.at[6 + i])
        for i, (src, dst) in enumerate(
            (
                (tokens, xs.at[0]),
                (mixer.at[own_rows, :], mix),
                (gains1, gain1),
                (gains2, gain2),
                (gains3, gain3.at[tp]),
            )
        )
    ]
    tall = (0, 1, 3, 4)
    fetch = {m: pltpu.make_async_copy(weights[m], raw.at[i], local_sem.at[11 + i]) for i, m in enumerate(tall)}
    for m in tall:
        fetch[m].start()
    for load in loads:
        load.start()

    def turn(group):
        for m in group:
            i = tall.index(m)
            fetch[m].wait()
            turned[i] = raw[i].T

    barrier = pltpu.get_barrier_semaphore()

    def greet(device):
        pl.semaphore_signal(barrier, inc=1, device_id=device, device_id_type=MESH)

    for k in range(1, PLANE):
        greet(relative(k))
    greet(partner)

    @pl.when(z > 0)
    def _():
        greet(down)

    @pl.when(z < depth - 1)
    def _():
        greet(up)

    below, above = (z + depth - 1) // depth, (2 * depth - 2 - z) // depth
    pl.semaphore_wait(barrier, PLANE + below + above)

    def own_part(m, which_y):
        at = pl.ds(pl.multiple_of((2 * rep + which_y) * width, SUBLANES), width)
        return weights[m].at[at, :] if m % 3 == 2 else turned.at[tall.index(m), at, :]

    def place(m, blk, half):
        at = pl.ds(pl.multiple_of(blk * block, block), block)
        held = dw.at[m // 3, half] if m % 3 == 2 else gu.at[m // 3, m % 3, half]
        return held.at[:, at]

    def remote(src, dst, send, recv, device):
        return pltpu.make_async_remote_copy(
            src_ref=src, dst_ref=dst, send_sem=send, recv_sem=recv, device_id=device, device_id_type=MESH
        )

    def keep(m):
        return pltpu.make_async_copy(own_part(m, y), place(m, fs, tp), local_sem.at[m])

    def swap(m):
        return remote(own_part(m, 1 - y), place(m, fs, tp), y_send.at[m], wide_recv.at[m, fs], relative(1))

    def send_up(m, blk, src):
        return remote(src, place(m, blk, tp), up_send.at[m, blk], wide_recv.at[m, blk], up)

    def send_down(m, blk, src):
        return remote(src, place(m, blk, tp), down_send.at[m, blk], wide_recv.at[m, blk], down)

    def send_core(m, blk, src):
        return remote(src, place(m, blk, tp), core_send.at[m, blk], core_recv.at[m, blk], partner)

    def came(m, blk):
        remote(place(m, blk, tp), place(m, blk, tp), core_send.at[m, blk], wide_recv.at[m, blk], partner).wait_recv()

    def came_core(m, blk):
        there = place(m, blk, 1 - tp)
        remote(there, there, core_send.at[m, blk], core_recv.at[m, blk], partner).wait_recv()

    def spread(m, blk, src, go_up=True, go_down=True):
        if go_up:

            @pl.when(z < depth - 1)
            def _():
                send_up(m, blk, src).start()

        if go_down:

            @pl.when(z > 0)
            def _():
                send_down(m, blk, src).start()

        send_core(m, blk, src).start()

    def begin(group):
        for m in group:
            keep(m).start()
            spread(m, fs, own_part(m, y))

    def from_side(group):
        other = 2 * z + (1 - y)
        for m in group:
            came(m, other)
            spread(m, other, place(m, other, tp))

    def from_line(group, d):
        for side in (y, 1 - y):
            for m in group:

                @pl.when(z >= d)
                def _():
                    blk = 2 * (z - d) + side
                    came(m, blk)
                    spread(m, blk, place(m, blk, tp), go_down=False)

                @pl.when(z + d < depth)
                def _():
                    blk = 2 * (z + d) + side
                    came(m, blk)
                    spread(m, blk, place(m, blk, tp), go_up=False)

    def ready(group):
        for m in group:
            keep(m).wait()
            for blk in range(2 * depth):
                came_core(m, blk)

    def rows_to(phase, k, src, dst):
        return remote(src, dst, row_send.at[phase, k], row_recv.at[phase, k], relative(k))

    def normalize_all(source, gain):
        gain_row = gain[...]

        def chunk(i, carry):
            normed[pl.ds(pl.multiple_of(i * rows, rows), rows), :] = norm_rows(source[i].astype(jnp.float32), gain_row)
            return carry

        lax.fori_loop(0, PLANE, chunk, 0)

    def inner(layer):
        def piece(i, carry):
            half, at = i // 2, pl.ds(pl.multiple_of((i % 2) * 2 * rows, 2 * rows), 2 * rows)
            columns = normed[at, :]
            gate = lax.dot_general(columns, gu[layer, 0, half], CROSS, preferred_element_type=jnp.float32)
            value = lax.dot_general(columns, gu[layer, 1, half], CROSS, preferred_element_type=jnp.float32)
            hidden = gate / (1.0 + jnp.exp(-gate)) * value
            hid[half, at, :] = hidden.astype(jnp.bfloat16)
            return carry

        lax.fori_loop(0, 4, piece, 0)

    def share_of(layer, k, zz):
        at = pl.ds(pl.multiple_of(zz * 2 * block, 2 * block), 2 * block)
        return remote(
            outgoing.at[layer, k, :, at],
            arrived.at[layer, k, :, at],
            part_send.at[layer, k, zz],
            part_recv.at[layer, k, zz],
            relative(k),
        )

    def outer(layer, zz):
        for which in range(2):
            came_core(3 * layer + 2, 2 * zz + which)
        at = pl.ds(pl.multiple_of(zz * 2 * block, 2 * block), 2 * block)
        part = jnp.dot(hid[0], dw[layer, 0, :, at], preferred_element_type=jnp.float32)
        part = part + jnp.dot(hid[1], dw[layer, 1, :, at], preferred_element_type=jnp.float32)
        for k in range(PLANE - 1, -1, -1):
            mine = part[k * rows : (k + 1) * rows]
            if k:
                outgoing[layer, k, :, at] = mine.astype(jnp.bfloat16)
                share_of(layer, k, zz).start()
            else:
                own[:, at] = mine

    def outer_at(layer, d):
        if d == 0:
            keep(3 * layer + 2).wait()
            outer(layer, z)
            return

        @pl.when(z >= d)
        def _():
            outer(layer, z - d)

        @pl.when(z + d < depth)
        def _():
            outer(layer, z + d)

    def rows_came(phase, dst):
        for k in range(1, PLANE):
            rows_to(phase, k, dst.at[k], dst.at[k]).wait_recv()

    def total(layer):
        for k in range(1, PLANE):
            for zz in range(depth):
                share_of(layer, k, zz).wait_recv()
        summed = own[...]
        for k in range(1, PLANE):
            summed = summed + arrived[layer, k].astype(jnp.float32)
        return summed

    one, two = (0, 1, 2), (3, 4, 5)
    swap_gain = remote(gains3, gain3.at[tp], end_sem.at[2], end_sem.at[3], partner)
    swap(2).start()
    begin(one[2:])
    turn(one[:2])
    for m in one[:2]:
        swap(m).start()
    begin(one[:2])
    for k in (3, 2, 1):
        rows_to(0, k, tokens, xs.at[k]).start()
    turn(two[:2])
    for m in two:
        swap(m).start()
    swap_gain.start()
    from_side((2, 0, 1))
    for d in range(1, depth):
        from_line((2, 0, 1), d)
    begin(two)
    from_side(two)
    for load in loads:
        load.wait()
    rows_came(0, xs)
    normalize_all(xs, gain1)
    ready(one[:2])
    inner(0)
    for d in range(depth):
        outer_at(0, d)
    if depth > 1:
        from_line(two[:2], 1)
    after_one = (xs[0].astype(jnp.float32) + 0.5 * total(0)).astype(jnp.bfloat16)
    mixed[0] = (after_one.astype(jnp.float32) + mix[...].astype(jnp.float32)).astype(jnp.bfloat16)
    for k in (3, 2, 1):
        rows_to(1, k, mixed.at[0], mixed.at[k]).start()
    for d in range(2, depth - 1):
        from_line(two[:2], d)
    if depth > 2:
        from_line(two[2:], 1)
    relays = (z > 0) & (z < depth - 1)

    @pl.when(relays)
    def _():
        for d in range(2, depth):
            from_line(two[2:], d)

    rows_came(1, mixed)
    normalize_all(mixed, gain2)
    if depth > 2:
        from_line(two[:2], depth - 1)
    elif depth > 1:
        from_line(two[2:], 1)
    ready(two[:2])
    inner(1)
    outer_at(1, 0)
    for d in range(1, depth):
        if d > 1:

            @pl.when((z == 0) | (z == depth - 1))
            def _():
                from_line(two[2:], d)

        outer_at(1, d)
    after_two = (mixed[0].astype(jnp.float32) + 0.5 * total(1)).astype(jnp.bfloat16)
    floats = after_two.astype(jnp.float32)
    floats = floats * lax.rsqrt(jnp.mean(floats * floats, axis=-1, keepdims=True) + EPS)
    share = width_all // 2
    swap_gain.wait_send()
    remote(gain3.at[1 - tp], gain3.at[1 - tp], end_sem.at[2], end_sem.at[3], partner).wait_recv()
    result[0] = (floats[:, :share] * gain3[0]).astype(jnp.bfloat16)
    result[1] = (floats[:, share:] * gain3[1]).astype(jnp.bfloat16)
    over = remote(result.at[1 - tp], landed, end_sem.at[0], end_sem.at[1], partner)
    over.start()
    out[own_rows, :] = result[tp]

    for m in range(6):
        swap(m).wait_send()
        for blk in range(2 * depth):
            send_core(m, blk, place(m, blk, tp)).wait_send()

            @pl.when((z < depth - 1) & (blk // 2 <= z))
            def _():
                send_up(m, blk, place(m, blk, tp)).wait_send()

            @pl.when((z > 0) & (blk // 2 >= z))
            def _():
                send_down(m, blk, place(m, blk, tp)).wait_send()

    for phase, src in enumerate((xs, mixed)):
        for k in range(1, PLANE):
            rows_to(phase, k, src.at[k], src.at[k]).wait_send()
            for zz in range(depth):
                share_of(phase, k, zz).wait_send()
    over.wait_send()
    over.wait_recv()
    out[pl.ds(pl.multiple_of((1 - tp) * rows, rows), rows), :] = landed[...]


def fused(
    tokens,
    mixer_out,
    gain_first,
    gate_first,
    up_first,
    down_first,
    gain_second,
    gate_second,
    up_second,
    down_second,
    gain_last,
):
    rows, features = tokens.shape
    block, hidden = gate_first.shape
    blocks = lax.axis_size("fs")
    if hidden % (PLANE * SUBLANES) or block % LANES or rows % SUBLANES:
        return local(
            tokens, mixer_out, gain_first, gate_first, up_first, down_first,
            gain_second, gate_second, up_second, down_second, gain_last,
        )
    width = hidden // PLANE
    vmem, anywhere = pl.BlockSpec(memory_space=pltpu.VMEM), pl.BlockSpec(memory_space=pltpu.HBM)
    half = jnp.bfloat16
    sems = pltpu.SemaphoreType.DMA
    return pl.pallas_call(
        functools.partial(kernel, blocks // 2, width),
        out_shape=jax.ShapeDtypeStruct((2 * rows, features // 2), half),
        in_specs=[anywhere] * 11,
        out_specs=vmem,
        scratch_shapes=[
            pltpu.VMEM((4, block, hidden), half),
            pltpu.VMEM((4, hidden, block), half),
            pltpu.VMEM((rows, features), half),
            pltpu.VMEM((1, features), jnp.float32),
            pltpu.VMEM((1, features), jnp.float32),
            pltpu.VMEM((2, 1, features // 2), jnp.float32),
            pltpu.VMEM((PLANE, rows, features), half),
            pltpu.VMEM((PLANE, rows, features), half),
            pltpu.VMEM((PLANE * rows, features), half),
            pltpu.VMEM((2, PLANE * rows, width), half),
            pltpu.VMEM((2, 2, 2, width, features), half),
            pltpu.VMEM((2, 2, width, features), half),
            pltpu.VMEM((2, PLANE, rows, features), half),
            pltpu.VMEM((2, PLANE, rows, features), half),
            pltpu.VMEM((rows, features), jnp.float32),
            pltpu.VMEM((2, rows, features // 2), half),
            pltpu.VMEM((rows, features // 2), half),
            sems((15,)),
            sems((6,)),
            sems((6, blocks)),
            sems((6, blocks)),
            sems((6, blocks)),
            sems((6, blocks)),
            sems((6, blocks)),
            sems((2, PLANE)),
            sems((2, PLANE)),
            sems((2, PLANE, blocks // 2)),
            sems((2, PLANE, blocks // 2)),
            sems((4,)),
        ],
        compiler_params=pltpu.CompilerParams(
            collective_id=0, has_side_effects=True, vmem_limit_bytes=67_043_328
        ),
    )(
        tokens,
        mixer_out,
        gain_first[None, :],
        gain_second[None, :],
        gain_last[None, :],
        gate_first,
        up_first,
        down_first,
        gate_second,
        up_second,
        down_second,
    )


def solution(mesh):
    in_specs = (
        P(("rep", "fs", "tp"), None),
        P(("rep", "fs"), None),
        P(),
        P("fs", "tp"),
        P("fs", "tp"),
        P("tp", "fs"),
        P(),
        P("fs", "tp"),
        P("fs", "tp"),
        P("tp", "fs"),
        P("tp"),
    )
    out_specs = P(("rep", "fs"), "tp")
    body = fused if fits(mesh) else local
    return jax.shard_map(body, mesh=mesh, in_specs=in_specs, out_specs=out_specs, check_vma=False)
```

```python
import functools

import jax
import jax.numpy as jnp
from jax import lax
from jax.experimental import pallas as pl
from jax.experimental.pallas import tpu as pltpu
from jax.sharding import PartitionSpec as P

EPS = 1e-06


def over_all(slab, axis, dim):

    def gathered(part):
        return lax.all_gather(part, axis, axis=dim, tiled=True)

    return jax.tree.map(gathered, slab)


def normalize(floats_in, gain_vec):
    floats = floats_in.astype(jnp.float32)
    factor = lax.rsqrt(jnp.mean(floats * floats, axis=-1, keepdims=True) + EPS)
    return (floats * factor * gain_vec.astype(jnp.float32)).astype(jnp.bfloat16)


def gather_group(row_block):
    return lax.all_gather(row_block, "tp", axis=0, tiled=True)


def inner_hidden(normed, w_gate, w_up):

    def add_both(totals, pieces):
        columns = lax.slice_in_dim(normed, 0, pieces[0].shape[0], axis=1)
        return (
            totals[0] + jnp.dot(columns, pieces[0], preferred_element_type=jnp.float32),
            totals[1] + jnp.dot(columns, pieces[1], preferred_element_type=jnp.float32),
        )

    empty = jnp.zeros((normed.shape[0], w_gate.shape[1]), jnp.float32)
    gate_acc, up_acc = add_both((empty, empty), over_all((w_gate, w_up), "fs", 0))
    return (jax.nn.silu(gate_acc) * up_acc).astype(jnp.bfloat16)


def outer_weight(w_down):
    return lax.all_gather(w_down, "fs", axis=1, tiled=True)


def local(
    tokens,
    mixer_out,
    gain_first,
    gate_first,
    up_first,
    down_first,
    gain_second,
    gate_second,
    up_second,
    down_second,
    gain_last,
):
    rows_dev = tokens.shape[0]
    tp_count = lax.axis_size("tp")
    tp_index = lax.axis_index("tp")
    normed_own = normalize(tokens, gain_first)
    normed_one = gather_group(normed_own)
    hidden_one = inner_hidden(normed_one, gate_first, up_first)
    down_full = outer_weight(down_first)

    def row_terms():
        picked = lax.slice_in_dim(hidden_one, 0, rows_dev * lax.axis_size("tp"), axis=0)
        return jnp.dot(picked, down_full, preferred_element_type=jnp.float32)

    ffn_one = lax.psum_scatter(
        row_terms().astype(jnp.bfloat16), "tp", scatter_dimension=0, tiled=True
    ).astype(jnp.float32)
    after_one = (tokens.astype(jnp.float32) + 0.5 * ffn_one).astype(jnp.bfloat16)
    own_mixer = lax.dynamic_slice_in_dim(mixer_out, tp_index * rows_dev, rows_dev, 0)
    mixed_in = (after_one.astype(jnp.float32) + own_mixer.astype(jnp.float32)).astype(jnp.bfloat16)
    gathered = gather_group(mixed_in)
    normed_two = normalize(gathered, gain_second)
    hidden_two = inner_hidden(normed_two, gate_second, up_second)
    down_two_full = outer_weight(down_second)
    terms_two = jnp.dot(hidden_two, down_two_full, preferred_element_type=jnp.float32)
    ffn_two = lax.psum_scatter(
        terms_two.astype(jnp.bfloat16), "tp", scatter_dimension=1, tiled=True
    ).astype(jnp.float32)
    col_width = ffn_two.shape[1]
    my_cols = lax.dynamic_slice_in_dim(gathered, tp_index * col_width, col_width, 1)
    after_two = (my_cols.astype(jnp.float32) + 0.5 * ffn_two).astype(jnp.bfloat16)
    floats = after_two.astype(jnp.float32)
    sum_sq = lax.psum(jnp.sum(floats * floats, axis=1), "tp")
    factor = lax.rsqrt(sum_sq / (col_width * tp_count) + EPS)
    return (floats * factor[:, None] * gain_last.astype(jnp.float32)[None, :]).astype(jnp.bfloat16)


MESH = pl.DeviceIdType.MESH
PLANE = 4
SUBLANES = 16
LANES = 128
CROSS = (((1,), (1,)), ((), ()))


def fits(mesh):
    return mesh.shape["rep"] == 2 and mesh.shape["tp"] == 2 and mesh.shape["fs"] % 2 == 0


def norm_rows(floats, gain_row):
    factor = lax.rsqrt(jnp.mean(floats * floats, axis=-1, keepdims=True) + EPS)
    return (floats * factor * gain_row).astype(jnp.bfloat16)


def kernel(
    depth, width,
    tokens, mixer, gains1, gains2, gains3, g1, u1, d1, g2, u2, d2,
    out,
    raw, turned, mix, gain1, gain2, gain3, xs, mixed, normed, hid, gu, dw, outgoing, arrived, own, result, landed,
    local_sem, y_send, up_send, down_send, wide_recv, core_send, core_recv,
    row_send, row_recv, part_send, part_recv, end_sem,
):
    rep, fs, tp = lax.axis_index("rep"), lax.axis_index("fs"), lax.axis_index("tp")
    z, y = fs // 2, fs % 2
    rows, width_all = tokens.shape
    block = g1.shape[0]
    weights = (g1, u1, d1, g2, u2, d2)
    partner = (rep, fs, 1 - tp)

    def relative(k):
        return ((rep + k // 2) % 2, 2 * z + (y + k % 2) % 2, tp)

    up, down = (rep, fs + 2, tp), (rep, fs - 2, tp)

    own_rows = pl.ds(pl.multiple_of(tp * rows, rows), rows)
    loads = [
        pltpu.make_async_copy(src, dst, local_sem.at[6 + i])
        for i, (src, dst) in enumerate(
            (
                (tokens, xs.at[0]),
                (mixer.at[own_rows, :], mix),
                (gains1, gain1),
                (gains2, gain2),
                (gains3, gain3.at[tp]),
            )
        )
    ]
    tall = (0, 1, 3, 4)
    fetch = {m: pltpu.make_async_copy(weights[m], raw.at[i], local_sem.at[11 + i]) for i, m in enumerate(tall)}
    for m in tall:
        fetch[m].start()
    for load in loads:
        load.start()

    def turn(group):
        for m in group:
            i = tall.index(m)
            fetch[m].wait()
            turned[i] = raw[i].T

    barrier = pltpu.get_barrier_semaphore()

    def greet(device):
        pl.semaphore_signal(barrier, inc=1, device_id=device, device_id_type=MESH)

    for k in range(1, PLANE):
        greet(relative(k))
    greet(partner)

    @pl.when(z > 0)
    def _():
        greet(down)

    @pl.when(z < depth - 1)
    def _():
        greet(up)

    below, above = (z + depth - 1) // depth, (2 * depth - 2 - z) // depth
    pl.semaphore_wait(barrier, PLANE + below + above)

    def own_part(m, which_y):
        at = pl.ds(pl.multiple_of((2 * rep + which_y) * width, SUBLANES), width)
        return weights[m].at[at, :] if m % 3 == 2 else turned.at[tall.index(m), at, :]

    def place(m, blk, half):
        at = pl.ds(pl.multiple_of(blk * block, block), block)
        held = dw.at[m // 3, half] if m % 3 == 2 else gu.at[m // 3, m % 3, half]
        return held.at[:, at]

    def remote(src, dst, send, recv, device):
        return pltpu.make_async_remote_copy(
            src_ref=src, dst_ref=dst, send_sem=send, recv_sem=recv, device_id=device, device_id_type=MESH
        )

    def keep(m):
        return pltpu.make_async_copy(own_part(m, y), place(m, fs, tp), local_sem.at[m])

    def swap(m):
        return remote(own_part(m, 1 - y), place(m, fs, tp), y_send.at[m], wide_recv.at[m, fs], relative(1))

    def send_up(m, blk, src):
        return remote(src, place(m, blk, tp), up_send.at[m, blk], wide_recv.at[m, blk], up)

    def send_down(m, blk, src):
        return remote(src, place(m, blk, tp), down_send.at[m, blk], wide_recv.at[m, blk], down)

    def send_core(m, blk, src):
        return remote(src, place(m, blk, tp), core_send.at[m, blk], core_recv.at[m, blk], partner)

    def came(m, blk):
        remote(place(m, blk, tp), place(m, blk, tp), core_send.at[m, blk], wide_recv.at[m, blk], partner).wait_recv()

    def came_core(m, blk):
        there = place(m, blk, 1 - tp)
        remote(there, there, core_send.at[m, blk], core_recv.at[m, blk], partner).wait_recv()

    def spread(m, blk, src, go_up=True, go_down=True):
        if go_up:

            @pl.when(z < depth - 1)
            def _():
                send_up(m, blk, src).start()

        if go_down:

            @pl.when(z > 0)
            def _():
                send_down(m, blk, src).start()

        send_core(m, blk, src).start()

    def begin(group):
        for m in group:
            keep(m).start()
            spread(m, fs, own_part(m, y))

    def from_side(group):
        other = 2 * z + (1 - y)
        for m in group:
            came(m, other)
            spread(m, other, place(m, other, tp))

    def from_line(group, d):
        for side in (y, 1 - y):
            for m in group:

                @pl.when(z >= d)
                def _():
                    blk = 2 * (z - d) + side
                    came(m, blk)
                    spread(m, blk, place(m, blk, tp), go_down=False)

                @pl.when(z + d < depth)
                def _():
                    blk = 2 * (z + d) + side
                    came(m, blk)
                    spread(m, blk, place(m, blk, tp), go_up=False)

    def ready(group):
        for m in group:
            keep(m).wait()
            for blk in range(2 * depth):
                came_core(m, blk)

    def rows_to(phase, k, src, dst):
        return remote(src, dst, row_send.at[phase, k], row_recv.at[phase, k], relative(k))

    def normalize_all(source, gain):
        gain_row = gain[...]

        def chunk(i, carry):
            normed[pl.ds(pl.multiple_of(i * rows, rows), rows), :] = norm_rows(source[i].astype(jnp.float32), gain_row)
            return carry

        lax.fori_loop(0, PLANE, chunk, 0)

    def inner(layer):
        def piece(i, carry):
            half, at = i // 2, pl.ds(pl.multiple_of((i % 2) * 2 * rows, 2 * rows), 2 * rows)
            columns = normed[at, :]
            gate = lax.dot_general(columns, gu[layer, 0, half], CROSS, preferred_element_type=jnp.float32)
            value = lax.dot_general(columns, gu[layer, 1, half], CROSS, preferred_element_type=jnp.float32)
            hidden = gate / (1.0 + jnp.exp(-gate)) * value
            hid[half, at, :] = hidden.astype(jnp.bfloat16)
            return carry

        lax.fori_loop(0, 4, piece, 0)

    def share_of(layer, k, zz):
        at = pl.ds(pl.multiple_of(zz * 2 * block, 2 * block), 2 * block)
        return remote(
            outgoing.at[layer, k, :, at],
            arrived.at[layer, k, :, at],
            part_send.at[layer, k, zz],
            part_recv.at[layer, k, zz],
            relative(k),
        )

    def outer(layer, zz):
        for which in range(2):
            came_core(3 * layer + 2, 2 * zz + which)
        at = pl.ds(pl.multiple_of(zz * 2 * block, 2 * block), 2 * block)
        part = jnp.dot(hid[0], dw[layer, 0, :, at], preferred_element_type=jnp.float32)
        part = part + jnp.dot(hid[1], dw[layer, 1, :, at], preferred_element_type=jnp.float32)
        for k in range(PLANE - 1, -1, -1):
            mine = part[k * rows : (k + 1) * rows]
            if k:
                outgoing[layer, k, :, at] = mine.astype(jnp.bfloat16)
                share_of(layer, k, zz).start()
            else:
                own[:, at] = mine

    def outer_at(layer, d):
        if d == 0:
            keep(3 * layer + 2).wait()
            outer(layer, z)
            return

        @pl.when(z >= d)
        def _():
            outer(layer, z - d)

        @pl.when(z + d < depth)
        def _():
            outer(layer, z + d)

    def rows_came(phase, dst):
        for k in range(1, PLANE):
            rows_to(phase, k, dst.at[k], dst.at[k]).wait_recv()

    def total(layer):
        for k in range(1, PLANE):
            for zz in range(depth):
                share_of(layer, k, zz).wait_recv()
        summed = own[...]
        for k in range(1, PLANE):
            summed = summed + arrived[layer, k].astype(jnp.float32)
        return summed

    one, two = (0, 1, 2), (3, 4, 5)
    relays = (z > 0) & (z < depth - 1)
    ends = (z == 0) | (z == depth - 1)
    swap_gain = remote(gains3, gain3.at[tp], end_sem.at[2], end_sem.at[3], partner)
    swap(2).start()
    begin(one[2:])
    turn(one[:2])
    for m in one[:2]:
        swap(m).start()
    begin(one[:2])
    for k in (3, 2, 1):
        rows_to(0, k, tokens, xs.at[k]).start()
    turn(two[:2])
    for m in two:
        swap(m).start()
    swap_gain.start()
    from_side(one)
    for d in range(1, depth):
        from_line(one[:2], d)

    @pl.when(relays)
    def _():
        for d in range(1, depth):
            from_line(one[2:], d)

    begin(two)
    from_side(two)
    for load in loads:
        load.wait()
    rows_came(0, xs)
    normalize_all(xs, gain1)
    ready(one[:2])
    inner(0)
    outer_at(0, 0)
    for d in range(1, depth):

        @pl.when(ends)
        def _():
            from_line(one[2:], d)

        outer_at(0, d)
    if depth > 1:
        from_line(two[:2], 1)
    after_one = (xs[0].astype(jnp.float32) + 0.5 * total(0)).astype(jnp.bfloat16)
    mixed[0] = (after_one.astype(jnp.float32) + mix[...].astype(jnp.float32)).astype(jnp.bfloat16)
    for k in (3, 2, 1):
        rows_to(1, k, mixed.at[0], mixed.at[k]).start()
    for d in range(2, depth - 1):
        from_line(two[:2], d)
    if depth > 2:
        from_line(two[2:], 1)
    @pl.when(relays)
    def _():
        for d in range(2, depth):
            from_line(two[2:], d)

    rows_came(1, mixed)
    normalize_all(mixed, gain2)
    if depth > 2:
        from_line(two[:2], depth - 1)
    elif depth > 1:
        from_line(two[2:], 1)
    ready(two[:2])
    inner(1)
    outer_at(1, 0)
    for d in range(1, depth):
        if d > 1:

            @pl.when(ends)
            def _():
                from_line(two[2:], d)

        outer_at(1, d)
    after_two = (mixed[0].astype(jnp.float32) + 0.5 * total(1)).astype(jnp.bfloat16)
    floats = after_two.astype(jnp.float32)
    floats = floats * lax.rsqrt(jnp.mean(floats * floats, axis=-1, keepdims=True) + EPS)
    share = width_all // 2
    swap_gain.wait_send()
    remote(gain3.at[1 - tp], gain3.at[1 - tp], end_sem.at[2], end_sem.at[3], partner).wait_recv()
    result[0] = (floats[:, :share] * gain3[0]).astype(jnp.bfloat16)
    result[1] = (floats[:, share:] * gain3[1]).astype(jnp.bfloat16)
    over = remote(result.at[1 - tp], landed, end_sem.at[0], end_sem.at[1], partner)
    over.start()
    out[own_rows, :] = result[tp]

    for m in range(6):
        swap(m).wait_send()
        for blk in range(2 * depth):
            send_core(m, blk, place(m, blk, tp)).wait_send()

            @pl.when((z < depth - 1) & (blk // 2 <= z))
            def _():
                send_up(m, blk, place(m, blk, tp)).wait_send()

            @pl.when((z > 0) & (blk // 2 >= z))
            def _():
                send_down(m, blk, place(m, blk, tp)).wait_send()

    for phase, src in enumerate((xs, mixed)):
        for k in range(1, PLANE):
            rows_to(phase, k, src.at[k], src.at[k]).wait_send()
            for zz in range(depth):
                share_of(phase, k, zz).wait_send()
    over.wait_send()
    over.wait_recv()
    out[pl.ds(pl.multiple_of((1 - tp) * rows, rows), rows), :] = landed[...]


def fused(
    tokens,
    mixer_out,
    gain_first,
    gate_first,
    up_first,
    down_first,
    gain_second,
    gate_second,
    up_second,
    down_second,
    gain_last,
):
    rows, features = tokens.shape
    block, hidden = gate_first.shape
    blocks = lax.axis_size("fs")
    if hidden % (PLANE * SUBLANES) or block % LANES or rows % SUBLANES:
        return local(
            tokens, mixer_out, gain_first, gate_first, up_first, down_first,
            gain_second, gate_second, up_second, down_second, gain_last,
        )
    width = hidden // PLANE
    vmem, anywhere = pl.BlockSpec(memory_space=pltpu.VMEM), pl.BlockSpec(memory_space=pltpu.HBM)
    half = jnp.bfloat16
    sems = pltpu.SemaphoreType.DMA
    return pl.pallas_call(
        functools.partial(kernel, blocks // 2, width),
        out_shape=jax.ShapeDtypeStruct((2 * rows, features // 2), half),
        in_specs=[anywhere] * 11,
        out_specs=vmem,
        scratch_shapes=[
            pltpu.VMEM((4, block, hidden), half),
            pltpu.VMEM((4, hidden, block), half),
            pltpu.VMEM((rows, features), half),
            pltpu.VMEM((1, features), jnp.float32),
            pltpu.VMEM((1, features), jnp.float32),
            pltpu.VMEM((2, 1, features // 2), jnp.float32),
            pltpu.VMEM((PLANE, rows, features), half),
            pltpu.VMEM((PLANE, rows, features), half),
            pltpu.VMEM((PLANE * rows, features), half),
            pltpu.VMEM((2, PLANE * rows, width), half),
            pltpu.VMEM((2, 2, 2, width, features), half),
            pltpu.VMEM((2, 2, width, features), half),
            pltpu.VMEM((2, PLANE, rows, features), half),
            pltpu.VMEM((2, PLANE, rows, features), half),
            pltpu.VMEM((rows, features), jnp.float32),
            pltpu.VMEM((2, rows, features // 2), half),
            pltpu.VMEM((rows, features // 2), half),
            sems((15,)),
            sems((6,)),
            sems((6, blocks)),
            sems((6, blocks)),
            sems((6, blocks)),
            sems((6, blocks)),
            sems((6, blocks)),
            sems((2, PLANE)),
            sems((2, PLANE)),
            sems((2, PLANE, blocks // 2)),
            sems((2, PLANE, blocks // 2)),
            sems((4,)),
        ],
        compiler_params=pltpu.CompilerParams(
            collective_id=0, has_side_effects=True, vmem_limit_bytes=67_043_328
        ),
    )(
        tokens,
        mixer_out,
        gain_first[None, :],
        gain_second[None, :],
        gain_last[None, :],
        gate_first,
        up_first,
        down_first,
        gate_second,
        up_second,
        down_second,
    )


def solution(mesh):
    in_specs = (
        P(("rep", "fs", "tp"), None),
        P(("rep", "fs"), None),
        P(),
        P("fs", "tp"),
        P("fs", "tp"),
        P("tp", "fs"),
        P(),
        P("fs", "tp"),
        P("fs", "tp"),
        P("tp", "fs"),
        P("tp"),
    )
    out_specs = P(("rep", "fs"), "tp")
    body = fused if fits(mesh) else local
    return jax.shard_map(body, mesh=mesh, in_specs=in_specs, out_specs=out_specs, check_vma=False)
```

```python
import functools

import jax
import jax.numpy as jnp
from jax import lax
from jax.experimental import pallas as pl
from jax.experimental.pallas import tpu as pltpu
from jax.sharding import PartitionSpec as P

EPS = 1e-06


def over_all(slab, axis, dim):

    def gathered(part):
        return lax.all_gather(part, axis, axis=dim, tiled=True)

    return jax.tree.map(gathered, slab)


def normalize(floats_in, gain_vec):
    floats = floats_in.astype(jnp.float32)
    factor = lax.rsqrt(jnp.mean(floats * floats, axis=-1, keepdims=True) + EPS)
    return (floats * factor * gain_vec.astype(jnp.float32)).astype(jnp.bfloat16)


def gather_group(row_block):
    return lax.all_gather(row_block, "tp", axis=0, tiled=True)


def inner_hidden(normed, w_gate, w_up):

    def add_both(totals, pieces):
        columns = lax.slice_in_dim(normed, 0, pieces[0].shape[0], axis=1)
        return (
            totals[0] + jnp.dot(columns, pieces[0], preferred_element_type=jnp.float32),
            totals[1] + jnp.dot(columns, pieces[1], preferred_element_type=jnp.float32),
        )

    empty = jnp.zeros((normed.shape[0], w_gate.shape[1]), jnp.float32)
    gate_acc, up_acc = add_both((empty, empty), over_all((w_gate, w_up), "fs", 0))
    return (jax.nn.silu(gate_acc) * up_acc).astype(jnp.bfloat16)


def outer_weight(w_down):
    return lax.all_gather(w_down, "fs", axis=1, tiled=True)


def local(
    tokens,
    mixer_out,
    gain_first,
    gate_first,
    up_first,
    down_first,
    gain_second,
    gate_second,
    up_second,
    down_second,
    gain_last,
):
    rows_dev = tokens.shape[0]
    tp_count = lax.axis_size("tp")
    tp_index = lax.axis_index("tp")
    normed_own = normalize(tokens, gain_first)
    normed_one = gather_group(normed_own)
    hidden_one = inner_hidden(normed_one, gate_first, up_first)
    down_full = outer_weight(down_first)

    def row_terms():
        picked = lax.slice_in_dim(hidden_one, 0, rows_dev * lax.axis_size("tp"), axis=0)
        return jnp.dot(picked, down_full, preferred_element_type=jnp.float32)

    ffn_one = lax.psum_scatter(
        row_terms().astype(jnp.bfloat16), "tp", scatter_dimension=0, tiled=True
    ).astype(jnp.float32)
    after_one = (tokens.astype(jnp.float32) + 0.5 * ffn_one).astype(jnp.bfloat16)
    own_mixer = lax.dynamic_slice_in_dim(mixer_out, tp_index * rows_dev, rows_dev, 0)
    mixed_in = (after_one.astype(jnp.float32) + own_mixer.astype(jnp.float32)).astype(jnp.bfloat16)
    gathered = gather_group(mixed_in)
    normed_two = normalize(gathered, gain_second)
    hidden_two = inner_hidden(normed_two, gate_second, up_second)
    down_two_full = outer_weight(down_second)
    terms_two = jnp.dot(hidden_two, down_two_full, preferred_element_type=jnp.float32)
    ffn_two = lax.psum_scatter(
        terms_two.astype(jnp.bfloat16), "tp", scatter_dimension=1, tiled=True
    ).astype(jnp.float32)
    col_width = ffn_two.shape[1]
    my_cols = lax.dynamic_slice_in_dim(gathered, tp_index * col_width, col_width, 1)
    after_two = (my_cols.astype(jnp.float32) + 0.5 * ffn_two).astype(jnp.bfloat16)
    floats = after_two.astype(jnp.float32)
    sum_sq = lax.psum(jnp.sum(floats * floats, axis=1), "tp")
    factor = lax.rsqrt(sum_sq / (col_width * tp_count) + EPS)
    return (floats * factor[:, None] * gain_last.astype(jnp.float32)[None, :]).astype(jnp.bfloat16)


MESH = pl.DeviceIdType.MESH
PLANE = 4
SUBLANES = 16
LANES = 128
CROSS = (((1,), (1,)), ((), ()))


def fits(mesh):
    return mesh.shape["rep"] == 2 and mesh.shape["tp"] == 2 and mesh.shape["fs"] % 2 == 0


def norm_rows(floats, gain_row):
    factor = lax.rsqrt(jnp.mean(floats * floats, axis=-1, keepdims=True) + EPS)
    return (floats * factor * gain_row).astype(jnp.bfloat16)


def kernel(
    depth, width,
    tokens, mixer, gains1, gains2, gains3, g1, u1, d1, g2, u2, d2,
    out,
    raw, turned, mix, gain1, gain2, gain3, xs, mixed, normed, hid, gu, dw, outgoing, arrived, own, result, landed,
    local_sem, y_send, up_send, down_send, wide_recv, core_send, core_recv,
    row_send, row_recv, part_send, part_recv, end_sem,
):
    rep, fs, tp = lax.axis_index("rep"), lax.axis_index("fs"), lax.axis_index("tp")
    z, y = fs // 2, fs % 2
    rows, width_all = tokens.shape
    block = g1.shape[0]
    weights = (g1, u1, d1, g2, u2, d2)
    partner = (rep, fs, 1 - tp)

    def relative(k):
        return ((rep + k // 2) % 2, 2 * z + (y + k % 2) % 2, tp)

    up, down = (rep, fs + 2, tp), (rep, fs - 2, tp)

    own_rows = pl.ds(pl.multiple_of(tp * rows, rows), rows)
    loads = [
        pltpu.make_async_copy(src, dst, local_sem.at[6 + i])
        for i, (src, dst) in enumerate(
            (
                (tokens, xs.at[0]),
                (mixer.at[own_rows, :], mix),
                (gains1, gain1),
                (gains2, gain2),
                (gains3, gain3.at[tp]),
            )
        )
    ]
    tall = (0, 1, 3, 4)
    fetch = {m: pltpu.make_async_copy(weights[m], raw.at[i], local_sem.at[11 + i]) for i, m in enumerate(tall)}
    for m in tall:
        fetch[m].start()
    for load in loads:
        load.start()

    def turn(group):
        for m in group:
            i = tall.index(m)
            fetch[m].wait()
            turned[i] = raw[i].T

    barrier = pltpu.get_barrier_semaphore()

    def greet(device):
        pl.semaphore_signal(barrier, inc=1, device_id=device, device_id_type=MESH)

    for k in range(1, PLANE):
        greet(relative(k))
    greet(partner)

    @pl.when(z > 0)
    def _():
        greet(down)

    @pl.when(z < depth - 1)
    def _():
        greet(up)

    below, above = (z + depth - 1) // depth, (2 * depth - 2 - z) // depth
    pl.semaphore_wait(barrier, PLANE + below + above)

    def own_part(m, which_y):
        at = pl.ds(pl.multiple_of((2 * rep + which_y) * width, SUBLANES), width)
        return weights[m].at[at, :] if m % 3 == 2 else turned.at[tall.index(m), at, :]

    def place(m, blk, half):
        at = pl.ds(pl.multiple_of(blk * block, block), block)
        held = dw.at[m // 3, half] if m % 3 == 2 else gu.at[m // 3, m % 3, half]
        return held.at[:, at]

    def remote(src, dst, send, recv, device):
        return pltpu.make_async_remote_copy(
            src_ref=src, dst_ref=dst, send_sem=send, recv_sem=recv, device_id=device, device_id_type=MESH
        )

    def keep(m):
        return pltpu.make_async_copy(own_part(m, y), place(m, fs, tp), local_sem.at[m])

    def swap(m):
        return remote(own_part(m, 1 - y), place(m, fs, tp), y_send.at[m], wide_recv.at[m, fs], relative(1))

    def send_up(m, blk, src):
        return remote(src, place(m, blk, tp), up_send.at[m, blk], wide_recv.at[m, blk], up)

    def send_down(m, blk, src):
        return remote(src, place(m, blk, tp), down_send.at[m, blk], wide_recv.at[m, blk], down)

    def send_core(m, blk, src):
        return remote(src, place(m, blk, tp), core_send.at[m, blk], core_recv.at[m, blk], partner)

    def came(m, blk):
        remote(place(m, blk, tp), place(m, blk, tp), core_send.at[m, blk], wide_recv.at[m, blk], partner).wait_recv()

    def came_core(m, blk):
        there = place(m, blk, 1 - tp)
        remote(there, there, core_send.at[m, blk], core_recv.at[m, blk], partner).wait_recv()

    def spread(m, blk, src, go_up=True, go_down=True):
        if go_up:

            @pl.when(z < depth - 1)
            def _():
                send_up(m, blk, src).start()

        if go_down:

            @pl.when(z > 0)
            def _():
                send_down(m, blk, src).start()

        send_core(m, blk, src).start()

    def begin(group):
        for m in group:
            keep(m).start()
            spread(m, fs, own_part(m, y))

    def from_side(group):
        other = 2 * z + (1 - y)
        for m in group:
            came(m, other)
            spread(m, other, place(m, other, tp))

    def from_line(group, d):
        for side in (y, 1 - y):
            for m in group:

                @pl.when(z >= d)
                def _():
                    blk = 2 * (z - d) + side
                    came(m, blk)
                    spread(m, blk, place(m, blk, tp), go_down=False)

                @pl.when(z + d < depth)
                def _():
                    blk = 2 * (z + d) + side
                    came(m, blk)
                    spread(m, blk, place(m, blk, tp), go_up=False)

    def ready(group):
        for m in group:
            keep(m).wait()
            for blk in range(2 * depth):
                came_core(m, blk)

    def rows_to(phase, k, src, dst):
        return remote(src, dst, row_send.at[phase, k, 0], row_recv.at[phase, k, 0], relative(k))

    def split_rows(held, there, k, h, via):
        at = pl.ds(h * (rows // 2), rows // 2)
        return remote(
            mixed.at[held, at, :], mixed.at[there, at, :], row_send.at[1, k, h], row_recv.at[1, k, h], relative(via)
        )

    def normalize_all(source, gain):
        gain_row = gain[...]

        def chunk(i, carry):
            normed[pl.ds(pl.multiple_of(i * rows, rows), rows), :] = norm_rows(source[i].astype(jnp.float32), gain_row)
            return carry

        lax.fori_loop(0, PLANE, chunk, 0)

    def inner(layer):
        def piece(i, carry):
            half, at = i // 2, pl.ds(pl.multiple_of((i % 2) * 2 * rows, 2 * rows), 2 * rows)
            columns = normed[at, :]
            gate = lax.dot_general(columns, gu[layer, 0, half], CROSS, preferred_element_type=jnp.float32)
            value = lax.dot_general(columns, gu[layer, 1, half], CROSS, preferred_element_type=jnp.float32)
            hidden = gate / (1.0 + jnp.exp(-gate)) * value
            hid[half, at, :] = hidden.astype(jnp.bfloat16)
            return carry

        lax.fori_loop(0, 4, piece, 0)

    def share_of(layer, k, zz):
        at = pl.ds(pl.multiple_of(zz * 2 * block, 2 * block), 2 * block)
        return remote(
            outgoing.at[layer, k, :, at],
            arrived.at[layer, k, :, at],
            part_send.at[layer, k, zz],
            part_recv.at[layer, k, zz],
            relative(k),
        )

    def outer(layer, zz):
        for which in range(2):
            came_core(3 * layer + 2, 2 * zz + which)
        at = pl.ds(pl.multiple_of(zz * 2 * block, 2 * block), 2 * block)
        part = jnp.dot(hid[0], dw[layer, 0, :, at], preferred_element_type=jnp.float32)
        part = part + jnp.dot(hid[1], dw[layer, 1, :, at], preferred_element_type=jnp.float32)
        for k in range(PLANE - 1, -1, -1):
            mine = part[k * rows : (k + 1) * rows]
            if k:
                outgoing[layer, k, :, at] = mine.astype(jnp.bfloat16)
                share_of(layer, k, zz).start()
            else:
                own[:, at] = mine

    def outer_at(layer, d):
        if d == 0:
            keep(3 * layer + 2).wait()
            outer(layer, z)
            return

        @pl.when(z >= d)
        def _():
            outer(layer, z - d)

        @pl.when(z + d < depth)
        def _():
            outer(layer, z + d)

    def rows_came(phase, dst):
        for k in range(1, PLANE):
            rows_to(phase, k, dst.at[k], dst.at[k]).wait_recv()

    def total(layer):
        for k in range(1, PLANE):
            for zz in range(depth):
                share_of(layer, k, zz).wait_recv()
        summed = own[...]
        for k in range(1, PLANE):
            summed = summed + arrived[layer, k].astype(jnp.float32)
        return summed

    one, two = (0, 1, 2), (3, 4, 5)
    relays = (z > 0) & (z < depth - 1)
    ends = (z == 0) | (z == depth - 1)
    swap_gain = remote(gains3, gain3.at[tp], end_sem.at[2], end_sem.at[3], partner)
    swap(2).start()
    begin(one[2:])
    turn(one[:2])
    for m in one[:2]:
        swap(m).start()
    begin(one[:2])
    for k in (3, 2, 1):
        rows_to(0, k, tokens, xs.at[k]).start()
    turn(two[:2])
    for m in two:
        swap(m).start()
    swap_gain.start()
    from_side(one)
    for d in range(1, depth):
        from_line(one[:2], d)

    @pl.when(relays)
    def _():
        for d in range(1, depth):
            from_line(one[2:], d)

    begin(two)
    from_side(two)
    for load in loads:
        load.wait()
    rows_came(0, xs)
    normalize_all(xs, gain1)
    ready(one[:2])
    inner(0)
    outer_at(0, 0)
    for d in range(1, depth):

        @pl.when(ends)
        def _():
            from_line(one[2:], d)

        outer_at(0, d)
    if depth > 1:
        from_line(two[:2], 1)
    after_one = (xs[0].astype(jnp.float32) + 0.5 * total(0)).astype(jnp.bfloat16)
    mixed[0] = (after_one.astype(jnp.float32) + mix[...].astype(jnp.float32)).astype(jnp.bfloat16)
    for h in range(2):
        split_rows(0, 2, 2, h, 2).start()
        split_rows(0, 1, 1, 1 - h, 1).start()
    split_rows(0, 2, 2, 0, 2).wait_recv()
    split_rows(2, 3, 3, 0, 1).start()
    split_rows(0, 1, 1, 1, 1).wait_recv()
    split_rows(1, 3, 3, 1, 2).start()
    for d in range(2, depth - 1):
        from_line(two[:2], d)
    if depth > 2:
        from_line(two[2:], 1)
    @pl.when(relays)
    def _():
        for d in range(2, depth):
            from_line(two[2:], d)

    split_rows(0, 2, 2, 1, 2).wait_recv()
    split_rows(0, 1, 1, 0, 1).wait_recv()
    split_rows(2, 3, 3, 0, 1).wait_recv()
    split_rows(1, 3, 3, 1, 2).wait_recv()
    normalize_all(mixed, gain2)
    if depth > 2:
        from_line(two[:2], depth - 1)
    elif depth > 1:
        from_line(two[2:], 1)
    ready(two[:2])
    inner(1)
    outer_at(1, 0)
    for d in range(1, depth):
        if d > 1:

            @pl.when(ends)
            def _():
                from_line(two[2:], d)

        outer_at(1, d)
    after_two = (mixed[0].astype(jnp.float32) + 0.5 * total(1)).astype(jnp.bfloat16)
    floats = after_two.astype(jnp.float32)
    floats = floats * lax.rsqrt(jnp.mean(floats * floats, axis=-1, keepdims=True) + EPS)
    share = width_all // 2
    swap_gain.wait_send()
    remote(gain3.at[1 - tp], gain3.at[1 - tp], end_sem.at[2], end_sem.at[3], partner).wait_recv()
    result[0] = (floats[:, :share] * gain3[0]).astype(jnp.bfloat16)
    result[1] = (floats[:, share:] * gain3[1]).astype(jnp.bfloat16)
    over = remote(result.at[1 - tp], landed, end_sem.at[0], end_sem.at[1], partner)
    over.start()
    out[own_rows, :] = result[tp]

    for m in range(6):
        swap(m).wait_send()
        for blk in range(2 * depth):
            send_core(m, blk, place(m, blk, tp)).wait_send()

            @pl.when((z < depth - 1) & (blk // 2 <= z))
            def _():
                send_up(m, blk, place(m, blk, tp)).wait_send()

            @pl.when((z > 0) & (blk // 2 >= z))
            def _():
                send_down(m, blk, place(m, blk, tp)).wait_send()

    for h in range(2):
        split_rows(0, 2, 2, h, 2).wait_send()
        split_rows(0, 1, 1, h, 1).wait_send()
        split_rows(2 - h, 3, 3, h, 1 + h).wait_send()
    for phase in range(2):
        for k in range(1, PLANE):
            if phase == 0:
                rows_to(phase, k, xs.at[k], xs.at[k]).wait_send()
            for zz in range(depth):
                share_of(phase, k, zz).wait_send()
    over.wait_send()
    over.wait_recv()
    out[pl.ds(pl.multiple_of((1 - tp) * rows, rows), rows), :] = landed[...]


def fused(
    tokens,
    mixer_out,
    gain_first,
    gate_first,
    up_first,
    down_first,
    gain_second,
    gate_second,
    up_second,
    down_second,
    gain_last,
):
    rows, features = tokens.shape
    block, hidden = gate_first.shape
    blocks = lax.axis_size("fs")
    if hidden % (PLANE * SUBLANES) or block % LANES or rows % SUBLANES:
        return local(
            tokens, mixer_out, gain_first, gate_first, up_first, down_first,
            gain_second, gate_second, up_second, down_second, gain_last,
        )
    width = hidden // PLANE
    vmem, anywhere = pl.BlockSpec(memory_space=pltpu.VMEM), pl.BlockSpec(memory_space=pltpu.HBM)
    half = jnp.bfloat16
    sems = pltpu.SemaphoreType.DMA
    return pl.pallas_call(
        functools.partial(kernel, blocks // 2, width),
        out_shape=jax.ShapeDtypeStruct((2 * rows, features // 2), half),
        in_specs=[anywhere] * 11,
        out_specs=vmem,
        scratch_shapes=[
            pltpu.VMEM((4, block, hidden), half),
            pltpu.VMEM((4, hidden, block), half),
            pltpu.VMEM((rows, features), half),
            pltpu.VMEM((1, features), jnp.float32),
            pltpu.VMEM((1, features), jnp.float32),
            pltpu.VMEM((2, 1, features // 2), jnp.float32),
            pltpu.VMEM((PLANE, rows, features), half),
            pltpu.VMEM((PLANE, rows, features), half),
            pltpu.VMEM((PLANE * rows, features), half),
            pltpu.VMEM((2, PLANE * rows, width), half),
            pltpu.VMEM((2, 2, 2, width, features), half),
            pltpu.VMEM((2, 2, width, features), half),
            pltpu.VMEM((2, PLANE, rows, features), half),
            pltpu.VMEM((2, PLANE, rows, features), half),
            pltpu.VMEM((rows, features), jnp.float32),
            pltpu.VMEM((2, rows, features // 2), half),
            pltpu.VMEM((rows, features // 2), half),
            sems((15,)),
            sems((6,)),
            sems((6, blocks)),
            sems((6, blocks)),
            sems((6, blocks)),
            sems((6, blocks)),
            sems((6, blocks)),
            sems((2, PLANE, 2)),
            sems((2, PLANE, 2)),
            sems((2, PLANE, blocks // 2)),
            sems((2, PLANE, blocks // 2)),
            sems((4,)),
        ],
        compiler_params=pltpu.CompilerParams(
            collective_id=0, has_side_effects=True, vmem_limit_bytes=67_043_328
        ),
    )(
        tokens,
        mixer_out,
        gain_first[None, :],
        gain_second[None, :],
        gain_last[None, :],
        gate_first,
        up_first,
        down_first,
        gate_second,
        up_second,
        down_second,
    )


def solution(mesh):
    in_specs = (
        P(("rep", "fs", "tp"), None),
        P(("rep", "fs"), None),
        P(),
        P("fs", "tp"),
        P("fs", "tp"),
        P("tp", "fs"),
        P(),
        P("fs", "tp"),
        P("fs", "tp"),
        P("tp", "fs"),
        P("tp"),
    )
    out_specs = P(("rep", "fs"), "tp")
    body = fused if fits(mesh) else local
    return jax.shard_map(body, mesh=mesh, in_specs=in_specs, out_specs=out_specs, check_vma=False)
```
